32 devices in a mesh: dp: 4 (over y, x), kv: 4 (over z), tp: 2 (over core).
Axes of the slice: x: 2, y: 2, z: 4, core: 2. Of those that a mesh axis runs over, the one named last changes fastest.
Arguments:
- incoming_vectors: bfloat16 [64, 4096], P('dp', ('kv', 'tp')), may hold values from -36 to 36
- mixer_scaling_vector: float32 [4096], P(('kv', 'tp')), may hold values from 0.1 to 1.9
- probe_matrix: bfloat16 [4096, 2048], P('kv', 'tp'), may hold values from -0.09375 to 0.09375
- address_matrix: bfloat16 [4096, 2048], P('kv', 'tp'), may hold values from -0.09375 to 0.09375
- content_matrix: bfloat16 [4096, 4096], P('kv', 'tp'), may hold values from -0.09375 to 0.09375
- result_sigmoid_matrix: bfloat16 [4096, 4096], P('kv', 'tp'), may hold values from -0.09375 to 0.09375
- storing_beta_matrix: bfloat16 [4096, 32], P('kv', 'tp'), may hold values from -0.09375 to 0.09375
- forgetting_matrix: bfloat16 [4096, 32], P('kv', 'tp'), may hold values from -0.09375 to 0.09375
- channel_forgetting_exponent: float32 [32], P('tp'), may hold values from -1 to 2
- forgetting_offset: float32 [32], P('tp'), may hold values from -3 to 0.5
- extra_forgetting: float32 [64, 32], P(('dp', 'kv'), 'tp'), may hold values from -0.7 to 0
- memory_matrices: float32 [64, 32, 128, 128], P(('dp', 'kv'), 'tp'), may hold values from -3 to 3
- channel_result_scaling: float32 [128], replicated, may hold values from 0.1 to 1.9
- mixer_exit_matrix: bfloat16 [4096, 4096], P('tp', 'kv'), may hold values from -0.09375 to 0.09375
- neuron_scaling_vector: float32 [4096], P(('kv', 'tp')), may hold values from 0.1 to 1.9
- widening_matrix: bfloat16 [4096, 16384], P(None, ('kv', 'tp')), may hold values from -0.09375 to 0.09375
- shrinking_matrix: bfloat16 [16384, 4096], P(('kv', 'tp')), may hold values from -0.0625 to 0.0625
Outputs:
- mixed: bfloat16 [64, 4096], P('dp', ('kv', 'tp'))
- new_state: float32 [64, 32, 128, 128], P(('dp', 'kv'), 'tp')
The draws below stay inside these ranges and needn't reach their ends.
All inputs are finite; a program needn't handle non-finite values.
Results may differ from the reference program's by a relative error of at most 0.018.
Values may be sent and summed in bfloat16 or wider, within the bound.
A program may use at most 128 MiB of HBM per device.

```python
import jax
import jax.numpy as jnp
from jax import lax

D = 4096
KHEADS = 16
CONTENT_SLOTS = 32
HEAD = 128
FF = 16384
STREAM_NUMBER = 64
N_KV = 4
N_TP = 2


def draw_incoming_vectors(key, part):
    first_key, second_key = jax.random.split(key, 2)
    columns = jnp.arange(D, dtype=jnp.float32) / D
    base = jnp.clip(jax.random.normal(first_key, (STREAM_NUMBER, D), jnp.float32), -6.0, 6.0)
    col_scale = 0.3 * 10.0 ** columns
    row_scale = jnp.exp(jax.random.uniform(second_key, (STREAM_NUMBER, 1), jnp.float32, jnp.log(0.5), jnp.log(2.0)))
    return (base * col_scale[None, :] * row_scale).astype(jnp.bfloat16)


def strengthened(entries, own_key, source, target, shards_of, factor):
    owner, partner = [(jnp.arange(entries.shape[axis_at]) // (entries.shape[axis_at] // shards_of)).reshape([-1 if axis == axis_at else 1 for axis in range(entries.ndim)]) for axis_at in (source, target)]
    chosen = jax.random.permutation(own_key, shards_of)[partner]
    strong = (owner == chosen) | (owner == (partner + shards_of // 2) % shards_of)
    return jnp.where(strong, factor * entries, entries)


def levels(key, extent, cuts, smallest, top_value):
    loudness = 1.0
    for dim, parts in cuts:
        draws = jax.random.uniform(jax.random.fold_in(jax.random.fold_in(key, 6), dim), (parts,), jnp.float32, smallest / len(cuts), top_value / len(cuts))
        loudness = loudness * jnp.repeat(jnp.exp(draws), extent[dim] // parts).reshape((-1,) + (1,) * (len(extent) - 1 - dim))
    return loudness


def noise(stream_key, extent, deviation, reach, pieces=(), held_as=jnp.bfloat16):
    result = jax.random.normal(stream_key, extent, jnp.float32) * deviation
    if len(pieces) > 0:
        result = levels(stream_key, extent, pieces, -0.22, 0.18) * result
    return jnp.clip(result, min=-reach, max=reach).astype(held_as)


def noise_with(key, extent, scale, bound, shards, heavy, kind=jnp.bfloat16):
    result = scale * jax.random.normal(key, extent, jnp.float32)
    if shards:
        result = result * levels(key, extent, shards, -0.22, 0.18)
    return jnp.clip(strengthened(result, jax.random.fold_in(key, 3), *heavy), -bound, bound).astype(kind)


def setup_inputs(seed: int = 0) -> dict:
    keys = jax.random.split(jax.random.key(seed), 18)
    incoming_vectors = draw_incoming_vectors(jax.random.fold_in(keys[17], 71), 0)
    mixer_scaling_vector = jnp.clip(1.0 + 0.18 * jax.random.normal(keys[1], (D,), jnp.float32), 0.1, 1.9)
    probe_matrix = noise(keys[2], (D, KHEADS * HEAD), D ** -0.5, 0.09375, ((0, 4), (1, 2)))
    address_matrix = noise(keys[3], (D, KHEADS * HEAD), D ** -0.5, 0.09375, ((0, 4), (1, 2)))
    content_matrix = noise(keys[4], (D, CONTENT_SLOTS * HEAD), D ** -0.5, 0.09375, ((0, 4), (1, 2)))
    result_sigmoid_matrix = noise(keys[5], (D, CONTENT_SLOTS * HEAD), D ** -0.5, 0.09375, ((0, 4), (1, 2)))
    storing_beta_matrix = noise(keys[6], (D, CONTENT_SLOTS), D ** -0.5, 0.09375, ((0, 4), (1, 2)))
    forgetting_matrix = noise(keys[7], (D, CONTENT_SLOTS), D ** -0.5, 0.09375, ((0, 4), (1, 2)))
    channel_forgetting_exponent = jnp.clip(-1.0 + 3.0 * jax.random.uniform(keys[8], (CONTENT_SLOTS,), jnp.float32) ** levels(keys[8], (CONTENT_SLOTS,), ((0, 2),), -0.2, 0.2), -1.0, 2.0)
    forgetting_offset = jnp.clip(-3.0 + 3.5 * jax.random.uniform(keys[9], (CONTENT_SLOTS,), jnp.float32) ** levels(keys[9], (CONTENT_SLOTS,), ((0, 2),), -0.2, 0.2), -3.0, 0.5)
    extra_forgetting = jnp.clip(-0.7 + 0.7 * jax.random.uniform(keys[10], (STREAM_NUMBER, CONTENT_SLOTS), jnp.float32) ** levels(keys[10], (STREAM_NUMBER, CONTENT_SLOTS), ((0, 16), (1, 2)), -0.2, 0.2), -0.7, 0.0)
    memory_matrices = noise(keys[11], (STREAM_NUMBER, CONTENT_SLOTS, HEAD, HEAD), 0.5, 3.0, ((0, 16), (1, 2)), jnp.float32)
    channel_result_scaling = jnp.clip(1.0 + 0.18 * jax.random.normal(keys[12], (HEAD,), jnp.float32), 0.1, 1.9)
    mixer_exit_matrix = noise(keys[13], (CONTENT_SLOTS * HEAD, D), (CONTENT_SLOTS * HEAD) ** -0.5, 0.09375, ((0, 2), (1, 4)))
    neuron_scaling_vector = jnp.clip(1.0 + 0.18 * jax.random.normal(keys[14], (D,), jnp.float32), 0.1, 1.9)
    widening_matrix = noise(keys[15], (D, FF), D ** -0.5, 0.09375, ((1, 8),))
    shrinking_matrix = noise_with(keys[16], (FF, D), FF ** -0.5, 0.0625, ((0, 8),), (0, 1, 8, 2.0))
    return {"incoming_vectors": incoming_vectors, "mixer_scaling_vector": mixer_scaling_vector, "probe_matrix": probe_matrix, "address_matrix": address_matrix, "content_matrix": content_matrix, "result_sigmoid_matrix": result_sigmoid_matrix, "storing_beta_matrix": storing_beta_matrix, "forgetting_matrix": forgetting_matrix, "channel_forgetting_exponent": channel_forgetting_exponent, "forgetting_offset": forgetting_offset, "extra_forgetting": extra_forgetting, "memory_matrices": memory_matrices, "channel_result_scaling": channel_result_scaling, "mixer_exit_matrix": mixer_exit_matrix, "neuron_scaling_vector": neuron_scaling_vector, "widening_matrix": widening_matrix, "shrinking_matrix": shrinking_matrix}


epsilon = 1e-06

def unit_norm(values):
    return values * lax.rsqrt(lax.optimization_barrier(jnp.sum(values * values, axis=-1, keepdims=True)) + epsilon)

def blocked_product(left, right, blocks):
    width = left.shape[1] // blocks
    total = jnp.zeros((left.shape[0], right.shape[1]), jnp.float32)
    for block in range(blocks):
        partial_sum = jnp.dot(left[:, block * width:(block + 1) * width], right[block * width:(block + 1) * width], preferred_element_type=jnp.float32)
        rounded = lax.optimization_barrier(partial_sum.astype(jnp.bfloat16))
        total = total + rounded.astype(jnp.float32)
    return total

def reference(incoming_vectors, mixer_scaling_vector, probe_matrix, address_matrix, content_matrix, result_sigmoid_matrix, storing_beta_matrix, forgetting_matrix, channel_forgetting_exponent, forgetting_offset, extra_forgetting, memory_matrices, channel_result_scaling, mixer_exit_matrix, neuron_scaling_vector, widening_matrix, shrinking_matrix):
    token_f = incoming_vectors.astype(jnp.float32)
    row_count = incoming_vectors.shape[0]
    inverse_root_mean = lax.rsqrt(lax.optimization_barrier(jnp.mean(token_f * token_f, axis=1, keepdims=True)) + epsilon)
    scaled = (token_f * mixer_scaling_vector).astype(jnp.bfloat16)

    def linear_transform(weight):
        return blocked_product(scaled, weight, N_KV) * inverse_root_mean
    repeat = CONTENT_SLOTS // KHEADS
    query = unit_norm(linear_transform(probe_matrix).reshape(row_count, KHEADS, HEAD)) * HEAD ** (-0.5)
    key_n = unit_norm(linear_transform(address_matrix).reshape(row_count, KHEADS, HEAD))
    query = jnp.repeat(query, repeat, axis=1)
    key_n = jnp.repeat(key_n, repeat, axis=1)
    value = linear_transform(content_matrix).reshape(row_count, CONTENT_SLOTS, HEAD)
    gate_raw = linear_transform(result_sigmoid_matrix).reshape(row_count, CONTENT_SLOTS, HEAD)
    beta = jax.nn.sigmoid(linear_transform(storing_beta_matrix))
    forgetting_exponent = -jnp.exp(channel_forgetting_exponent) * jax.nn.softplus(linear_transform(forgetting_matrix) + forgetting_offset) + extra_forgetting
    decayed = jnp.exp(forgetting_exponent)[:, :, None, None] * memory_matrices
    predicted = jnp.einsum('shde,shd->she', decayed, key_n, precision=lax.Precision.HIGHEST)
    new_state = decayed + beta[:, :, None, None] * key_n[:, :, :, None] * (value - predicted)[:, :, None, :]
    head_out = jnp.einsum('shde,shd->she', new_state, query, precision=lax.Precision.HIGHEST)
    normed = head_out * lax.rsqrt(lax.optimization_barrier(jnp.mean(head_out * head_out, axis=-1, keepdims=True)) + epsilon)
    gated = (normed * channel_result_scaling * jax.nn.silu(gate_raw)).astype(jnp.bfloat16).reshape(row_count, CONTENT_SLOTS * HEAD)
    attn = blocked_product(gated, mixer_exit_matrix, N_TP)
    resid = (token_f + attn).astype(jnp.bfloat16)
    resid_f = resid.astype(jnp.float32)
    inv_rms2 = lax.rsqrt(lax.optimization_barrier(jnp.mean(resid_f * resid_f, axis=1, keepdims=True)) + epsilon)
    scaled2 = (resid_f * neuron_scaling_vector).astype(jnp.bfloat16)
    up_raw = jax.nn.relu(jnp.dot(scaled2, widening_matrix, preferred_element_type=jnp.float32) * inv_rms2)
    hidden = (up_raw * up_raw).astype(jnp.bfloat16)
    mixed = (resid_f + blocked_product(hidden, shrinking_matrix, N_KV * N_TP)).astype(jnp.bfloat16)
    return (mixed, new_state)
```

```python
import functools

import jax
import jax.numpy as jnp
from jax import lax
from jax.experimental import pallas as pl
from jax.experimental.pallas import tpu as pltpu
from jax.sharding import PartitionSpec as P

MESH = pl.DeviceIdType.MESH
EPS = 1e-06
F32 = jnp.float32
BF16 = jnp.bfloat16


def dot(left, right):
    return jnp.dot(left, right, preferred_element_type=F32)


def layer(
    KV, TP, D,
    x, g1, wq, wk, wv, wg, wb, wd, fexp, foff, extra, mem, crs, wo, g2, wu, ws,
    mixed, new_state,
    xb, g1b, g2b, vq, vk, vv, vg, vb, vd, vfexp, vfoff, vextra, st, vcrs, vo, vu, vs,
    qst, qrc, vst, vrc, gst, grc, sst, src, kq, ho, gall, ap, rb, up, hid, dst, drc, mo,
    lsem, usem, ssem, osem,
    bs, br, x_s, x_r, p_s, p_r, a_s, a_r, t_s, t_r, r_s, r_r, d_s, d_r,
):
    kv, tp = lax.axis_index("kv"), lax.axis_index("tp")
    N = KV * TP
    flat = kv * TP + tp
    R, C = x.shape
    own = R // KV
    K1 = TP * C
    heads = st.shape[1]
    HEAD = st.shape[2]
    khe = wq.shape[1] // HEAD
    rep = heads // khe
    QC, VC = wq.shape[1], wv.shape[1]

    def local(i, a, b):
        c = pltpu.make_async_copy(a, b, lsem.at[i])
        c.start()
        return c

    cx = local(0, x, xb.at[tp])
    cg1 = local(1, g1, g1b.at[tp])
    cg2 = local(2, g2, g2b.at[flat])
    cq = local(3, wq, vq)
    ck = local(4, wk, vk)
    cb = local(5, wb, vb)
    cd = local(6, wd, vd)
    cv = local(7, wv, vv)
    cg = local(8, wg, vg)
    smalls = [
        local(9, fexp, vfexp), local(10, foff, vfoff), local(11, extra, vextra),
        local(12, crs, vcrs),
    ]

    barrier = pltpu.get_barrier_semaphore()
    for s in range(1, N):
        other = lax.rem(flat + s, N)
        pl.semaphore_signal(
            barrier, inc=1, device_id={"kv": other // TP, "tp": lax.rem(other, TP)},
            device_id_type=MESH,
        )
    pl.semaphore_wait(barrier, N - 1)

    def remote(a, b, ss, rs, okv, otp):
        return pltpu.make_async_remote_copy(
            src_ref=a, dst_ref=b, send_sem=ss, recv_sem=rs,
            device_id={"kv": okv, "tp": otp}, device_id_type=MESH,
        )

    sends = []
    for s in range(1, TP):
        o = lax.rem(tp + s, TP)
        c = remote(x, xb.at[tp], x_s.at[0, o], x_r.at[0, tp], kv, o)
        c.start()
        sends.append(c)
        c = remote(g1, g1b.at[tp], x_s.at[1, o], x_r.at[1, tp], kv, o)
        c.start()
        sends.append(c)
    for s in range(1, N):
        o = lax.rem(flat + s, N)
        c = remote(g2, g2b.at[flat], bs.at[o], br.at[flat], o // TP, lax.rem(o, TP))
        c.start()
        sends.append(c)
    cst = local(13, mem, st)
    co = local(14, wo, vo)

    cx.wait()
    cg1.wait()
    for s in range(1, TP):
        o = lax.rem(tp + s, TP)
        remote(x, xb.at[o], x_s.at[0, o], x_r.at[0, o], kv, o).wait_recv()
        remote(g1, g1b.at[o], x_s.at[1, o], x_r.at[1, o], kv, o).wait_recv()
    xf = jnp.concatenate([xb[t] for t in range(TP)], axis=1).astype(F32)
    gf = jnp.concatenate([g1b[t] for t in range(TP)], axis=1)
    scaled = (xf * gf).astype(BF16)
    ssq = jnp.broadcast_to(jnp.sum(xf * xf, axis=1, keepdims=True), (R, 128))
    for p in range(KV):
        sst[p] = ssq[p * own:(p + 1) * own]

    def scatter(stage, rec, i):
        for s in range(1, KV):
            o = lax.rem(kv + s, KV)
            c = remote(stage.at[o], rec.at[kv], p_s.at[i, o], p_r.at[i, kv], o, tp)
            c.start()
            sends.append(c)
        rec[kv] = stage[kv]

    def arrive(stage, rec, i):
        for s in range(1, KV):
            o = lax.rem(kv + s, KV)
            remote(stage.at[o], rec.at[o], p_s.at[i, o], p_r.at[i, o], o, tp).wait_recv()
        total = rec[0].astype(F32)
        for p in range(1, KV):
            total = total + rec[p].astype(F32)
        return total

    scatter(sst, src, 0)

    def project(w, stage, base):
        cols = w.shape[1]
        step = min(cols, 1024)
        for c in range(cols // step):
            part = dot(scaled, w[:, c * step:(c + 1) * step])
            for p in range(KV):
                stage[p, :, base + c * step:base + (c + 1) * step] = part[
                    p * own:(p + 1) * own
                ].astype(BF16)

    cq.wait()
    project(vq, qst, 0)
    ck.wait()
    project(vk, qst, QC)
    ups = []
    for s in range(KV):
        o = lax.rem(kv + s, KV)
        rows = pl.ds(pl.multiple_of(o * K1, K1), K1)
        c = pltpu.make_async_copy(wu.at[rows], vu.at[rows], usem.at[s])
        c.start()
        ups.append(c)
    cb.wait()
    cd.wait()
    project(vb, qst, 2 * QC)
    project(vd, qst, 2 * QC + 128)
    scatter(qst, qrc, 1)
    cv.wait()
    project(vv, vst, 0)
    scatter(vst, vrc, 2)
    downs = []
    SR = ws.shape[0] // 4
    for s in range(4):
        rows = pl.ds(s * SR, SR)
        c = pltpu.make_async_copy(ws.at[rows], vs.at[rows], ssem.at[s])
        c.start()
        downs.append(c)
    cg.wait()
    project(vg, gst, 0)
    scatter(gst, grc, 3)

    for c in smalls:
        c.wait()
    inv = lax.rsqrt(arrive(sst, src, 0)[:, 0:1] * (1.0 / D) + EPS)
    qk = arrive(qst, qrc, 1) * inv
    beta = jax.nn.sigmoid(qk[:, 2 * QC:2 * QC + heads])
    z = qk[:, 2 * QC + 128:2 * QC + 128 + heads] + vfoff[...]
    soft = jnp.maximum(z, 0.0) + jnp.log1p(jnp.exp(-jnp.abs(z)))
    decay = jnp.exp(vextra[...] - jnp.exp(vfexp[...]) * soft)
    kqd = []
    half = khe * own
    for h in range(khe):
        q_h = qk[:, h * HEAD:(h + 1) * HEAD]
        k_h = qk[:, QC + h * HEAD:QC + (h + 1) * HEAD]
        q_h = q_h * (
            lax.rsqrt(jnp.sum(q_h * q_h, axis=1, keepdims=True) + EPS) * HEAD ** (-0.5)
        )
        k_h = k_h * lax.rsqrt(jnp.sum(k_h * k_h, axis=1, keepdims=True) + EPS)
        kqd.append(jnp.sum(q_h * k_h, axis=1, keepdims=True))
        kq[h * own:(h + 1) * own, :] = k_h
        kq[half + h * own:half + (h + 1) * own, :] = q_h
    kqt = jnp.transpose(kq[...])
    value = arrive(vst, vrc, 2) * inv
    cst.wait()
    outs = []
    for hk in range(khe):
        for s in range(own):
            i = hk * own + s
            kcol = kqt[:, i:i + 1]
            qcol = kqt[:, half + i:half + i + 1]
            kd = kqd[hk][s:s + 1]
            for r in range(rep):
                h = hk * rep + r
                S = st[s, h]
                a = decay[s:s + 1, h:h + 1]
                pk = jnp.sum(S * kcol, axis=0, keepdims=True)
                pq = jnp.sum(S * qcol, axis=0, keepdims=True)
                u = beta[s:s + 1, h:h + 1] * (
                    value[s:s + 1, h * HEAD:(h + 1) * HEAD] - a * pk
                )
                ho[s:s + 1, h * HEAD:(h + 1) * HEAD] = a * pq + kd * u
                st[s, h] = a * S + kcol * u
        hs = pl.ds(hk * rep, rep)
        c = pltpu.make_async_copy(st.at[:, hs], new_state.at[:, hs], osem.at[hk])
        c.start()
        outs.append(c)

    gate = arrive(gst, grc, 3) * inv
    for h in range(heads):
        cols = slice(h * HEAD, (h + 1) * HEAD)
        o_h = ho[:, cols]
        v = gate[:, cols]
        n_h = o_h * lax.rsqrt(jnp.mean(o_h * o_h, axis=1, keepdims=True) + EPS)
        gall[kv, :, cols] = (n_h * vcrs[...] * (v / (1.0 + jnp.exp(-v)))).astype(BF16)
    for s in range(1, KV):
        o = lax.rem(kv + s, KV)
        c = remote(gall.at[kv], gall.at[kv], a_s.at[o], a_r.at[kv], o, tp)
        c.start()
        sends.append(c)
    co.wait()
    for s in range(1, KV):
        o = lax.rem(kv + s, KV)
        remote(gall.at[o], gall.at[o], a_s.at[o], a_r.at[o], o, tp).wait_recv()
    gated = jnp.concatenate([gall[p].astype(F32) for p in range(KV)], axis=0).astype(BF16)
    ap[tp] = dot(gated, vo[...]).astype(BF16)
    for s in range(1, TP):
        o = lax.rem(tp + s, TP)
        c = remote(ap.at[tp], ap.at[tp], t_s.at[o], t_r.at[tp], kv, o)
        c.start()
        sends.append(c)
    for s in range(1, TP):
        o = lax.rem(tp + s, TP)
        remote(ap.at[o], ap.at[o], t_s.at[o], t_r.at[o], kv, o).wait_recv()
    attn = ap[0].astype(F32)
    for t in range(1, TP):
        attn = attn + ap[t].astype(F32)
    xf = jnp.concatenate([xb[t] for t in range(TP)], axis=1).astype(F32)
    rb[kv] = (xf + attn).astype(BF16)
    for s in range(1, KV):
        o = lax.rem(kv + s, KV)
        c = remote(rb.at[kv], rb.at[kv], r_s.at[o], r_r.at[kv], o, tp)
        c.start()
        sends.append(c)

    cg2.wait()
    for s in range(1, N):
        o = lax.rem(flat + s, N)
        remote(g2, g2b.at[o], bs.at[o], br.at[o], o // TP, lax.rem(o, TP)).wait_recv()
    ssq2 = jnp.zeros((R, 1), F32)
    UC = wu.shape[1]
    ustep = min(UC, 1024)
    for s in range(KV):
        o = lax.rem(kv + s, KV)
        if s:
            remote(rb.at[o], rb.at[o], r_s.at[o], r_r.at[o], o, tp).wait_recv()
        ups[s].wait()
        res = rb[o].astype(F32)
        ssq2 = ssq2 + jnp.sum(res * res, axis=1, keepdims=True)
        gain = jnp.concatenate([g2b[o * TP + t] for t in range(TP)], axis=1)
        sc = (res * gain).astype(BF16)
        rows = pl.ds(pl.multiple_of(o * K1, K1), K1)
        for c in range(UC // ustep):
            cols = slice(c * ustep, (c + 1) * ustep)
            part = dot(sc, vu[rows, cols])
            if s:
                part = part + up[:, cols]
            up[:, cols] = part
    inv2 = lax.rsqrt(ssq2 * (1.0 / D) + EPS)
    hv = jnp.maximum(up[...] * inv2, 0.0)
    hid[...] = (hv * hv).astype(BF16)
    for c in downs:
        c.wait()

    def down(t, carry):
        i, j = t // TP, lax.rem(t, TP)
        step = (i + 1) // 2
        okv = lax.rem(
            kv + KV // 2 + jnp.where(lax.rem(i, 2) == 0, step, -step) + KV, KV
        )
        otp = lax.rem(tp + TP - 1 - j, TP)
        o = okv * TP + otp
        part = dot(hid[...], vs[:, pl.ds(pl.multiple_of(o * C, C), C)])
        dst[o] = part.astype(BF16)

        @pl.when(t < N - 1)
        def _():
            remote(dst.at[o], drc.at[flat], d_s.at[o], d_r.at[flat], okv, otp).start()

        return carry

    lax.fori_loop(0, N, down, 0)
    total = rb[kv, :, pl.ds(pl.multiple_of(tp * C, C), C)].astype(F32) + dst[flat].astype(F32)
    for s in range(1, N):
        o = lax.rem(flat + s, N)
        remote(dst.at[o], drc.at[o], d_s.at[o], d_r.at[o], o // TP, lax.rem(o, TP)).wait_recv()
        total = total + drc[o].astype(F32)
    mo[...] = total.astype(BF16)
    last = pltpu.make_async_copy(mo, mixed, osem.at[khe])
    last.start()
    for c in sends:
        c.wait_send()
    for s in range(1, N):
        o = lax.rem(flat + s, N)
        remote(dst.at[o], drc.at[o], d_s.at[o], d_r.at[o], o // TP, lax.rem(o, TP)).wait_send()
    for c in outs:
        c.wait()
    last.wait()


def solution(mesh):
    KV, TP = mesh.shape["kv"], mesh.shape["tp"]

    def on_device(x, g1, wq, wk, wv, wg, wb, wd, fexp, foff, extra, mem, crs, wo, g2, wu, ws):
        R, C = x.shape
        N = KV * TP
        D = C * N
        own, heads, HEAD, _ = mem.shape
        QC, VC = wq.shape[1], wv.shape[1]
        khe = QC // HEAD
        K1 = C * TP
        V = pltpu.VMEM
        S = pltpu.SemaphoreType.DMA
        args = (
            x, g1[None], wq, wk, wv, wg, wb, wd, fexp[None], foff[None], extra, mem,
            crs[None], wo, g2[None], wu, ws,
        )
        kqr = -(-2 * khe * own // 128) * 128
        scratch = [
            V((TP, R, C), BF16), V((TP, 1, C), F32), V((N, 1, C), F32),
            V(wq.shape, BF16), V(wk.shape, BF16), V(wv.shape, BF16), V(wg.shape, BF16),
            V(wb.shape, BF16), V(wd.shape, BF16),
            V((1, heads), F32), V((1, heads), F32), V(extra.shape, F32),
            V(mem.shape, F32), V((1, HEAD), F32),
            V(wo.shape, BF16), V(wu.shape, BF16), V(ws.shape, BF16),
            V((KV, own, 2 * QC + 256), BF16), V((KV, own, 2 * QC + 256), BF16),
            V((KV, own, VC), BF16), V((KV, own, VC), BF16),
            V((KV, own, VC), BF16), V((KV, own, VC), BF16),
            V((KV, own, 128), F32), V((KV, own, 128), F32),
            V((kqr, HEAD), F32), V((own, VC), F32),
            V((KV, own, VC), BF16), V((TP, R, K1), BF16), V((KV, R, K1), BF16),
            V((R, wu.shape[1]), F32), V((R, wu.shape[1]), BF16),
            V((N, R, C), BF16), V((N, R, C), BF16), V((R, C), BF16),
            S((15,)), S((KV,)), S((4,)), S((khe + 1,)),
            S((N,)), S((N,)), S((2, TP)), S((2, TP)), S((4, KV)), S((4, KV)),
            S((KV,)), S((KV,)), S((TP,)), S((TP,)), S((KV,)), S((KV,)), S((N,)), S((N,)),
        ]
        any_spec = pl.BlockSpec(memory_space=pl.ANY)
        return pl.pallas_call(
            functools.partial(layer, KV, TP, D),
            out_shape=(
                jax.ShapeDtypeStruct((R, C), BF16),
                jax.ShapeDtypeStruct(mem.shape, F32),
            ),
            in_specs=[any_spec] * len(args),
            out_specs=(any_spec, any_spec),
            scratch_shapes=scratch,
            compiler_params=pltpu.CompilerParams(
                collective_id=0, has_side_effects=True, vmem_limit_bytes=67043328
            ),
            name="layer",
        )(*args)

    return jax.shard_map(
        on_device,
        mesh=mesh,
        in_specs=(
            P("dp", ("kv", "tp")),
            P(("kv", "tp")),
            P("kv", "tp"),
            P("kv", "tp"),
            P("kv", "tp"),
            P("kv", "tp"),
            P("kv", "tp"),
            P("kv", "tp"),
            P("tp"),
            P("tp"),
            P(("dp", "kv"), "tp"),
            P(("dp", "kv"), "tp", None, None),
            P(),
            P("tp", "kv"),
            P(("kv", "tp")),
            P(None, ("kv", "tp")),
            P(("kv", "tp"), None),
        ),
        out_specs=(P("dp", ("kv", "tp")), P(("dp", "kv"), "tp", None, None)),
        check_vma=False,
    )
```

```python
import functools

import jax
import jax.numpy as jnp
from jax import lax
from jax.experimental import pallas as pl
from jax.experimental.pallas import tpu as pltpu
from jax.sharding import PartitionSpec as P

MESH = pl.DeviceIdType.MESH
EPS = 1e-06
F32 = jnp.float32
BF16 = jnp.bfloat16
VMEM_LIMIT = 58 << 20


def dot(left, right):
    return jnp.dot(left, right, preferred_element_type=F32)


def layer(
    KV, TP, D,
    x, g1, wq, wk, wv, wg, wb, wd, fexp, foff, extra, mem, crs, wo, g2, wu, ws,
    mo, st,
    xb, g1b, g2b, vq, vk, vv, vg, vb, vd, vfexp, vfoff, vextra, vcrs, vo, vu, vs,
    qst, qrc, vst, vrc, gst, grc, sst, src, kq, ho, gall, ap, rb, up, hid, dst, drc, pacc,
    lsem, usem, ssem,
    bs, br, x_s, x_r, p_s, p_r, a_s, a_r, t_s, t_r, r_s, r_r, d_s, d_r,
):
    kv, tp = lax.axis_index("kv"), lax.axis_index("tp")
    N = KV * TP
    flat = kv * TP + tp
    R, C = x.shape
    own = R // KV
    K1 = TP * C
    heads = st.shape[1]
    HEAD = st.shape[2]
    khe = wq.shape[1] // HEAD
    rep = heads // khe
    QC, VC = wq.shape[1], wv.shape[1]

    def local(i, a, b):
        c = pltpu.make_async_copy(a, b, lsem.at[i])
        c.start()
        return c

    cx = local(0, x, xb.at[tp])
    cg1 = local(1, g1, g1b.at[tp])
    cg2 = local(2, g2, g2b.at[flat])
    cq = local(3, wq, vq)
    ck = local(4, wk, vk)
    cb = local(5, wb, vb)
    cd = local(6, wd, vd)
    cv = local(7, wv, vv)
    cg = local(8, wg, vg)
    smalls = [
        local(9, fexp, vfexp), local(10, foff, vfoff), local(11, extra, vextra),
        local(12, crs, vcrs),
    ]

    barrier = pltpu.get_barrier_semaphore()
    for s in range(1, N):
        other = lax.rem(flat + s, N)
        pl.semaphore_signal(
            barrier, inc=1, device_id={"kv": other // TP, "tp": lax.rem(other, TP)},
            device_id_type=MESH,
        )
    pl.semaphore_wait(barrier, N - 1)

    def remote(a, b, ss, rs, okv, otp):
        return pltpu.make_async_remote_copy(
            src_ref=a, dst_ref=b, send_sem=ss, recv_sem=rs,
            device_id={"kv": okv, "tp": otp}, device_id_type=MESH,
        )

    sends = []
    for s in range(1, TP):
        o = lax.rem(tp + s, TP)
        c = remote(x, xb.at[tp], x_s.at[0, o], x_r.at[0, tp], kv, o)
        c.start()
        sends.append(c)
        c = remote(g1, g1b.at[tp], x_s.at[1, o], x_r.at[1, tp], kv, o)
        c.start()
        sends.append(c)
    for s in range(1, N):
        o = lax.rem(flat + s, N)
        c = remote(g2, g2b.at[flat], bs.at[o], br.at[flat], o // TP, lax.rem(o, TP))
        c.start()
        sends.append(c)
    cx.wait()
    cg1.wait()
    mine = (xb[tp].astype(F32) * g1b[tp]).astype(BF16)

    def first(w, base):
        cols = w.shape[1]
        step = min(cols, 1024)
        rows = pl.ds(pl.multiple_of(tp * C, C), C)
        for c in range(cols // step):
            pacc[:, base + c * step:base + (c + 1) * step] = dot(
                mine, w[rows, c * step:(c + 1) * step]
            )

    cq.wait()
    first(vq, 0)
    ck.wait()
    first(vk, QC)
    cst = local(13, mem, st)
    co = local(14, wo, vo)
    for s in range(1, TP):
        o = lax.rem(tp + s, TP)
        remote(x, xb.at[o], x_s.at[0, o], x_r.at[0, o], kv, o).wait_recv()
        remote(g1, g1b.at[o], x_s.at[1, o], x_r.at[1, o], kv, o).wait_recv()
    xf = jnp.concatenate([xb[t] for t in range(TP)], axis=1).astype(F32)
    gf = jnp.concatenate([g1b[t] for t in range(TP)], axis=1)
    scaled = (xf * gf).astype(BF16)
    ssq = jnp.broadcast_to(jnp.sum(xf * xf, axis=1, keepdims=True), (R, 128))
    for p in range(KV):
        sst[p] = ssq[p * own:(p + 1) * own]

    def scatter(stage, rec, i):
        for s in range(1, KV):
            o = lax.rem(kv + s, KV)
            c = remote(stage.at[o], rec.at[kv], p_s.at[i, o], p_r.at[i, kv], o, tp)
            c.start()
            sends.append(c)
        rec[kv] = stage[kv]

    def arrive(stage, rec, i):
        for s in range(1, KV):
            o = lax.rem(kv + s, KV)
            remote(stage.at[o], rec.at[o], p_s.at[i, o], p_r.at[i, o], o, tp).wait_recv()
        total = rec[0].astype(F32)
        for p in range(1, KV):
            total = total + rec[p].astype(F32)
        return total

    scatter(sst, src, 0)

    def rest(w, stage, base):
        cols = w.shape[1]
        step = min(cols, 1024)
        for c in range(cols // step):
            part = pacc[:, base + c * step:base + (c + 1) * step]
            for s in range(1, TP):
                o = lax.rem(tp + s, TP)
                x_o = (xb[o].astype(F32) * g1b[o]).astype(BF16)
                rows = pl.ds(pl.multiple_of(o * C, C), C)
                part = part + dot(x_o, w[rows, c * step:(c + 1) * step])
            for p in range(KV):
                stage[p, :, base + c * step:base + (c + 1) * step] = part[
                    p * own:(p + 1) * own
                ].astype(BF16)

    def small(w, stage, base):
        part = lax.dot_general(
            scaled, w[...], (((1,), (1,)), ((), ())), preferred_element_type=F32
        )
        for p in range(KV):
            stage[p, :, base:base + heads] = part[p * own:(p + 1) * own].astype(BF16)

    def project(w, stage, base):
        cols = w.shape[1]
        step = min(cols, 1024)
        for c in range(cols // step):
            part = dot(scaled, w[:, c * step:(c + 1) * step])
            for p in range(KV):
                stage[p, :, base + c * step:base + (c + 1) * step] = part[
                    p * own:(p + 1) * own
                ].astype(BF16)

    rest(vq, qst, 0)
    rest(vk, qst, QC)
    cb.wait()
    cd.wait()
    small(vb, qst, 2 * QC)
    small(vd, qst, 2 * QC + 128)
    scatter(qst, qrc, 1)
    cv.wait()
    ups = []
    for s in range(KV):
        o = lax.rem(kv + s, KV)
        rows = pl.ds(pl.multiple_of(o * K1, K1), K1)
        c = pltpu.make_async_copy(wu.at[rows], vu.at[rows], usem.at[s])
        c.start()
        ups.append(c)
    project(vv, vst, 0)
    scatter(vst, vrc, 2)
    cg.wait()
    downs = []
    SR = ws.shape[0] // 4
    for s in range(4):
        rows = pl.ds(s * SR, SR)
        c = pltpu.make_async_copy(ws.at[rows], vs.at[rows], ssem.at[s])
        c.start()
        downs.append(c)
    project(vg, gst, 0)
    scatter(gst, grc, 3)

    for c in smalls:
        c.wait()
    inv = lax.rsqrt(arrive(sst, src, 0)[:, 0:1] * (1.0 / D) + EPS)
    qk = arrive(qst, qrc, 1) * inv
    beta = jax.nn.sigmoid(qk[:, 2 * QC:2 * QC + heads])
    z = qk[:, 2 * QC + 128:2 * QC + 128 + heads] + vfoff[...]
    soft = jnp.maximum(z, 0.0) + jnp.log1p(jnp.exp(-jnp.abs(z)))
    decay = jnp.exp(vextra[...] - jnp.exp(vfexp[...]) * soft)
    kqd = []
    half = khe * own
    for h in range(khe):
        q_h = qk[:, h * HEAD:(h + 1) * HEAD]
        k_h = qk[:, QC + h * HEAD:QC + (h + 1) * HEAD]
        q_h = q_h * (
            lax.rsqrt(jnp.sum(q_h * q_h, axis=1, keepdims=True) + EPS) * HEAD ** (-0.5)
        )
        k_h = k_h * lax.rsqrt(jnp.sum(k_h * k_h, axis=1, keepdims=True) + EPS)
        kqd.append(jnp.sum(q_h * k_h, axis=1, keepdims=True))
        kq[h * own:(h + 1) * own, :] = k_h
        kq[half + h * own:half + (h + 1) * own, :] = q_h
    kqt = jnp.transpose(kq[...])
    value = arrive(vst, vrc, 2) * inv
    cst.wait()
    for hk in range(khe):
        for s in range(own):
            i = hk * own + s
            kcol = kqt[:, i:i + 1]
            qcol = kqt[:, half + i:half + i + 1]
            kd = kqd[hk][s:s + 1]
            for r in range(rep):
                h = hk * rep + r
                S = st[s, h]
                a = decay[s:s + 1, h:h + 1]
                pk = jnp.sum(S * kcol, axis=0, keepdims=True)
                pq = jnp.sum(S * qcol, axis=0, keepdims=True)
                u = beta[s:s + 1, h:h + 1] * (
                    value[s:s + 1, h * HEAD:(h + 1) * HEAD] - a * pk
                )
                ho[s:s + 1, h * HEAD:(h + 1) * HEAD] = a * pq + kd * u
                st[s, h] = a * S + kcol * u

    gate = arrive(gst, grc, 3) * inv
    for h in range(heads):
        cols = slice(h * HEAD, (h + 1) * HEAD)
        o_h = ho[:, cols]
        v = gate[:, cols]
        n_h = o_h * lax.rsqrt(jnp.mean(o_h * o_h, axis=1, keepdims=True) + EPS)
        gall[kv, :, cols] = (n_h * vcrs[...] * (v / (1.0 + jnp.exp(-v)))).astype(BF16)
    for s in range(1, KV):
        o = lax.rem(kv + s, KV)
        c = remote(gall.at[kv], gall.at[kv], a_s.at[o], a_r.at[kv], o, tp)
        c.start()
        sends.append(c)
    co.wait()
    for s in range(1, KV):
        o = lax.rem(kv + s, KV)
        remote(gall.at[o], gall.at[o], a_s.at[o], a_r.at[o], o, tp).wait_recv()
    gated = jnp.concatenate([gall[p].astype(F32) for p in range(KV)], axis=0).astype(BF16)
    ap[tp] = dot(gated, vo[...]).astype(BF16)
    for s in range(1, TP):
        o = lax.rem(tp + s, TP)
        c = remote(ap.at[tp], ap.at[tp], t_s.at[o], t_r.at[tp], kv, o)
        c.start()
        sends.append(c)
    for s in range(1, TP):
        o = lax.rem(tp + s, TP)
        remote(ap.at[o], ap.at[o], t_s.at[o], t_r.at[o], kv, o).wait_recv()
    attn = ap[0].astype(F32)
    for t in range(1, TP):
        attn = attn + ap[t].astype(F32)
    xf = jnp.concatenate([xb[t] for t in range(TP)], axis=1).astype(F32)
    rb[kv] = (xf + attn).astype(BF16)
    for s in range(1, KV):
        o = lax.rem(kv + s, KV)
        c = remote(rb.at[kv], rb.at[kv], r_s.at[o], r_r.at[kv], o, tp)
        c.start()
        sends.append(c)

    cg2.wait()
    for s in range(1, N):
        o = lax.rem(flat + s, N)
        remote(g2, g2b.at[o], bs.at[o], br.at[o], o // TP, lax.rem(o, TP)).wait_recv()
    ssq2 = jnp.zeros((R, 1), F32)
    UC = wu.shape[1]
    ustep = min(UC, 1024)
    for s in range(KV):
        o = lax.rem(kv + s, KV)
        if s:
            remote(rb.at[o], rb.at[o], r_s.at[o], r_r.at[o], o, tp).wait_recv()
        ups[s].wait()
        res = rb[o].astype(F32)
        ssq2 = ssq2 + jnp.sum(res * res, axis=1, keepdims=True)
        gain = jnp.concatenate([g2b[o * TP + t] for t in range(TP)], axis=1)
        sc = (res * gain).astype(BF16)
        rows = pl.ds(pl.multiple_of(o * K1, K1), K1)
        for c in range(UC // ustep):
            cols = slice(c * ustep, (c + 1) * ustep)
            part = dot(sc, vu[rows, cols])
            if s:
                part = part + up[:, cols]
            up[:, cols] = part
    inv2 = lax.rsqrt(ssq2 * (1.0 / D) + EPS)
    hv = jnp.maximum(up[...] * inv2, 0.0)
    hid[...] = (hv * hv).astype(BF16)
    for c in downs:
        c.wait()

    def down(t, carry):
        i, j = t // TP, lax.rem(t, TP)
        step = (i + 1) // 2
        okv = lax.rem(
            kv + KV // 2 + jnp.where(lax.rem(i, 2) == 0, step, -step) + KV, KV
        )
        otp = lax.rem(tp + TP - 1 - j, TP)
        o = okv * TP + otp
        part = dot(hid[...], vs[:, pl.ds(pl.multiple_of(o * C, C), C)])
        dst[o] = part.astype(BF16)

        @pl.when(t < N - 1)
        def _():
            remote(dst.at[o], drc.at[flat], d_s.at[o], d_r.at[flat], okv, otp).start()

        return carry

    lax.fori_loop(0, N, down, 0)
    total = rb[kv, :, pl.ds(pl.multiple_of(tp * C, C), C)].astype(F32) + dst[flat].astype(F32)
    for s in range(1, N):
        o = lax.rem(flat + s, N)
        remote(dst.at[o], drc.at[o], d_s.at[o], d_r.at[o], o // TP, lax.rem(o, TP)).wait_recv()
        total = total + drc[o].astype(F32)
    mo[...] = total.astype(BF16)
    for c in sends:
        c.wait_send()
    for s in range(1, N):
        o = lax.rem(flat + s, N)
        remote(dst.at[o], drc.at[o], d_s.at[o], d_r.at[o], o // TP, lax.rem(o, TP)).wait_send()


def solution(mesh):
    KV, TP = mesh.shape["kv"], mesh.shape["tp"]

    def on_device(x, g1, wq, wk, wv, wg, wb, wd, fexp, foff, extra, mem, crs, wo, g2, wu, ws):
        R, C = x.shape
        N = KV * TP
        D = C * N
        own, heads, HEAD, _ = mem.shape
        QC, VC = wq.shape[1], wv.shape[1]
        khe = QC // HEAD
        K1 = C * TP
        V = pltpu.VMEM
        S = pltpu.SemaphoreType.DMA
        args = (
            x, g1[None], wq, wk, wv, wg, wb.T, wd.T, fexp[None], foff[None], extra, mem,
            crs[None], wo, g2[None], wu, ws,
        )
        kqr = -(-2 * khe * own // 128) * 128
        scratch = [
            V((TP, R, C), BF16), V((TP, 1, C), F32), V((N, 1, C), F32),
            V(wq.shape, BF16), V(wk.shape, BF16), V(wv.shape, BF16), V(wg.shape, BF16),
            V(wb.shape[::-1], BF16), V(wd.shape[::-1], BF16),
            V((1, heads), F32), V((1, heads), F32), V(extra.shape, F32),
            V((1, HEAD), F32),
            V(wo.shape, BF16), V(wu.shape, BF16), V(ws.shape, BF16),
            V((KV, own, 2 * QC + 256), BF16), V((KV, own, 2 * QC + 256), BF16),
            V((KV, own, VC), BF16), V((KV, own, VC), BF16),
            V((KV, own, VC), BF16), V((KV, own, VC), BF16),
            V((KV, own, 128), F32), V((KV, own, 128), F32),
            V((kqr, HEAD), F32), V((own, VC), F32),
            V((KV, own, VC), BF16), V((TP, R, K1), BF16), V((KV, R, K1), BF16),
            V((R, wu.shape[1]), F32), V((R, wu.shape[1]), BF16),
            V((N, R, C), BF16), V((N, R, C), BF16), V((R, 2 * QC), F32),
            S((15,)), S((KV,)), S((4,)),
            S((N,)), S((N,)), S((2, TP)), S((2, TP)), S((4, KV)), S((4, KV)),
            S((KV,)), S((KV,)), S((TP,)), S((TP,)), S((KV,)), S((KV,)), S((N,)), S((N,)),
        ]
        any_spec = pl.BlockSpec(memory_space=pl.ANY)
        return pl.pallas_call(
            functools.partial(layer, KV, TP, D),
            out_shape=(
                pltpu.VMEM((R, C), BF16),
                pltpu.VMEM(mem.shape, F32),
            ),
            in_specs=[any_spec] * len(args),
            out_specs=(pl.BlockSpec(memory_space=pltpu.VMEM),) * 2,
            scratch_shapes=scratch,
            compiler_params=pltpu.CompilerParams(
                collective_id=0, has_side_effects=True, vmem_limit_bytes=VMEM_LIMIT
            ),
            name="layer",
        )(*args)

    return jax.shard_map(
        on_device,
        mesh=mesh,
        in_specs=(
            P("dp", ("kv", "tp")),
            P(("kv", "tp")),
            P("kv", "tp"),
            P("kv", "tp"),
            P("kv", "tp"),
            P("kv", "tp"),
            P("kv", "tp"),
            P("kv", "tp"),
            P("tp"),
            P("tp"),
            P(("dp", "kv"), "tp"),
            P(("dp", "kv"), "tp", None, None),
            P(),
            P("tp", "kv"),
            P(("kv", "tp")),
            P(None, ("kv", "tp")),
            P(("kv", "tp"), None),
        ),
        out_specs=(P("dp", ("kv", "tp")), P(("dp", "kv"), "tp", None, None)),
        check_vma=False,
    )
```
